32 devices in a mesh: rep: 2 (over x), fs: 8 (over z, y), tp: 2 (over core).
Axes of the slice: x: 2, y: 2, z: 4, core: 2. Of those that a mesh axis runs over, the one named last changes fastest.
Arguments:
- tokens: bfloat16 [8192, 2048], P(('rep', 'fs')), may hold values from -6 to 6
- mix_gain: bfloat16 [2048], replicated, may hold values from 0.099609375 to 1.8984375
- value_weight: bfloat16 [2048, 1536], P('fs', 'tp'), may hold values from -0.125 to 0.125
- outer_gate_weight: bfloat16 [2048, 1536], P('fs', 'tp'), may hold values from -0.125 to 0.125
- inner_gate_weight: bfloat16 [2048, 1536], P('fs', 'tp'), may hold values from -0.125 to 0.125
- conv_taps: bfloat16 [3, 1536], P(None, 'tp'), may hold values from -3 to 3
- mix_out_weight: bfloat16 [1536, 2048], P('tp', 'fs'), may hold values from -0.15625 to 0.15625
- ffn_gain: bfloat16 [2048], replicated, may hold values from 0.099609375 to 1.8984375
- gate_weight: bfloat16 [2048, 4096], P('fs', 'tp'), may hold values from -0.125 to 0.125
- up_weight: bfloat16 [2048, 4096], P('fs', 'tp'), may hold values from -0.125 to 0.125
- down_weight: bfloat16 [4096, 2048], P('tp', 'fs'), may hold values from -0.09375 to 0.09375
Outputs:
- layer_out: bfloat16 [8192, 2048], P(('rep', 'fs'))
The draws below stay inside these ranges and needn't reach their ends.
All inputs are finite; a program needn't handle non-finite values.
Results may differ from the reference program's by a relative error of at most 0.02.
Values may be sent and summed in bfloat16 or wider, within the bound.
A program may use at most 128 MiB of HBM per device.

```python
import jax
import jax.numpy as jnp
from jax import lax

D = 2048
C = 1536
FF = 4096
TAPS = 3
SEQ_GRP = 2
ROWS = 512
TOKENS = 8192
N_TP = 2


def levels(own_key, extent, pieces, least, largest):
    level = 1.0
    for dim, parts in pieces:
        draws = jax.random.uniform(jax.random.fold_in(jax.random.fold_in(own_key, 6), dim), (parts,), jnp.float32, least / len(pieces), largest / len(pieces))
        level = level * jnp.repeat(jnp.exp(draws), extent[dim] // parts).reshape((-1,) + (1,) * (len(extent) - 1 - dim))
    return level


def gaussian(key, shape, spread, limit, shards=(), held_as=jnp.bfloat16):
    level = levels(key, shape, shards, -0.22, 0.18) if shards else 1.0
    entries = jax.random.normal(key, shape, jnp.float32) * spread * level
    return jnp.minimum(jnp.maximum(entries, -limit), limit).astype(held_as)


def setup_inputs(seed: int = 0) -> dict:
    splits = jax.random.split(jax.random.key(seed), 12)
    return {
        "tokens": gaussian(splits[0], (TOKENS, D), 1.0, 6.0, ((0, 16),)),
        "mix_gain": jnp.clip(1.0 + 0.18 * jax.random.normal(splits[1], (D,), jnp.float32), 0.099609375, 1.8984375).astype(jnp.bfloat16),
        "value_weight": gaussian(splits[2], (D, C), D ** -0.5, 0.125, ((0, 8), (1, 2))),
        "outer_gate_weight": gaussian(splits[3], (D, C), D ** -0.5, 0.125, ((0, 8), (1, 2))),
        "inner_gate_weight": gaussian(splits[4], (D, C), D ** -0.5, 0.125, ((0, 8), (1, 2))),
        "conv_taps": gaussian(splits[5], (TAPS, C), 0.58, 3.0, ((1, 2),)),
        "mix_out_weight": gaussian(splits[6], (C, D), C ** -0.5, 0.15625, ((0, 2), (1, 8))),
        "ffn_gain": jnp.clip(1.0 + 0.18 * jax.random.normal(splits[7], (D,), jnp.float32), 0.099609375, 1.8984375).astype(jnp.bfloat16),
        "gate_weight": gaussian(splits[8], (D, FF), D ** -0.5, 0.125, ((0, 8), (1, 2))),
        "up_weight": gaussian(splits[9], (D, FF), D ** -0.5, 0.125, ((0, 8), (1, 2))),
        "down_weight": gaussian(splits[10], (FF, D), FF ** -0.5, 0.09375, ((0, 2), (1, 8))),
    }


EPS = 1e-05

def rms_norm(values, gain):
    floats = values.astype(jnp.float32)
    scaled = floats * lax.rsqrt(lax.optimization_barrier(jnp.mean(floats * floats, axis=-1, keepdims=True)) + EPS)
    return (scaled * gain.astype(jnp.float32)).astype(jnp.bfloat16)

def short_conv(value_proj, outer_proj, inner_proj, conv_taps, seq_len):
    mixed_in = inner_proj.astype(jnp.float32) * value_proj.astype(jnp.float32)
    count_rows = mixed_in.shape[0]
    position = (jnp.arange(count_rows, dtype=jnp.int32) % seq_len)[:, None]
    zero_row = jnp.zeros((1, mixed_in.shape[1]), jnp.float32)
    back_one = jnp.where(position >= 1, jnp.concatenate([zero_row, mixed_in[:-1]], axis=0), 0.0)
    back_two = jnp.where(position >= 2, jnp.concatenate([zero_row, zero_row, mixed_in[:-2]], axis=0), 0.0)
    taps = conv_taps.astype(jnp.float32)
    convolved = taps[0] * back_two + taps[1] * back_one + taps[2] * mixed_in
    return (outer_proj.astype(jnp.float32) * convolved).astype(jnp.bfloat16)

def split_sum(left, right, groups):
    group_cols = left.shape[1] // groups
    summed = jnp.zeros((left.shape[0], right.shape[1]), jnp.float32)
    for shard_number in range(groups):
        low = shard_number * group_cols
        partial_value = jnp.dot(left[:, low:low + group_cols], right[low:low + group_cols], preferred_element_type=jnp.float32).astype(jnp.bfloat16)
        partial_value = lax.optimization_barrier(partial_value)
        summed = summed + partial_value.astype(jnp.float32)
    return summed

def reference(tokens, mix_gain, value_weight, outer_gate_weight, inner_gate_weight, conv_taps, mix_out_weight, ffn_gain, gate_weight, up_weight, down_weight):
    seq_len = ROWS // SEQ_GRP
    normed = rms_norm(tokens, mix_gain)
    value_proj = jnp.dot(normed, value_weight, preferred_element_type=jnp.float32).astype(jnp.bfloat16)
    outer_proj = jnp.dot(normed, outer_gate_weight, preferred_element_type=jnp.float32).astype(jnp.bfloat16)
    inner_proj = jnp.dot(normed, inner_gate_weight, preferred_element_type=jnp.float32).astype(jnp.bfloat16)
    mixed = short_conv(value_proj, outer_proj, inner_proj, conv_taps, seq_len)
    after_mix = (tokens.astype(jnp.float32) + split_sum(mixed, mix_out_weight, N_TP)).astype(jnp.bfloat16)
    normed_two = rms_norm(after_mix, ffn_gain)
    gate_proj = jnp.dot(normed_two, gate_weight, preferred_element_type=jnp.float32)
    up_proj = jnp.dot(normed_two, up_weight, preferred_element_type=jnp.float32)
    hidden = (jax.nn.silu(gate_proj) * up_proj).astype(jnp.bfloat16)
    return (after_mix.astype(jnp.float32) + split_sum(hidden, down_weight, N_TP)).astype(jnp.bfloat16)
```

```python
import jax
import jax.numpy as jnp
from jax import lax
from jax.sharding import PartitionSpec as P

SEQ_GRP = 2


EPS = 1e-05


def rms_norm(values, gain):
    floats = values.astype(jnp.float32)
    scaled = floats * lax.rsqrt(jnp.mean(floats * floats, axis=-1, keepdims=True) + EPS)
    return (scaled * gain.astype(jnp.float32)).astype(jnp.bfloat16)


def short_conv(value_proj, outer_proj, inner_proj, conv_taps, seq_len):
    mixed_in = inner_proj.astype(jnp.float32) * value_proj.astype(jnp.float32)
    count_rows = mixed_in.shape[0]
    position = (jnp.arange(count_rows, dtype=jnp.int32) % seq_len)[:, None]
    zero_row = jnp.zeros((1, mixed_in.shape[1]), jnp.float32)
    back_one = jnp.where(position >= 1, jnp.concatenate([zero_row, mixed_in[:-1]], axis=0), 0.0)
    back_two = jnp.where(
        position >= 2, jnp.concatenate([zero_row, zero_row, mixed_in[:-2]], axis=0), 0.0
    )
    taps = conv_taps.astype(jnp.float32)
    convolved = taps[0] * back_two + taps[1] * back_one + taps[2] * mixed_in
    return (outer_proj.astype(jnp.float32) * convolved).astype(jnp.bfloat16)


def shifted(values, axis, step):
    size = lax.axis_size(axis)
    return lax.ppermute(values, axis, [(i, (i + step) % size) for i in range(size)])


def spread(block, axis):
    size, me, rows = lax.axis_size(axis), lax.axis_index(axis), block.shape[0]
    if size == 2:
        other = shifted(block, axis, 1)
        first = me == 0
        return jnp.concatenate([jnp.where(first, block, other), jnp.where(first, other, block)])
    whole = jnp.zeros((size * rows,) + block.shape[1:], block.dtype)
    for step in range(size):
        piece = block if step == 0 else shifted(block, axis, step)
        whole = lax.dynamic_update_slice_in_dim(whole, piece, (me - step) % size * rows, 0)
    return whole


def by_rep(block):
    return [block] + [shifted(block, "rep", step) for step in range(1, lax.axis_size("rep"))]


def group_rows(share_block):
    return jnp.concatenate([spread(block, "tp") for block in by_rep(share_block)])


def reduce_rows(partial, share):
    n_tp, tp, n_rep = lax.axis_size("tp"), lax.axis_index("tp"), lax.axis_size("rep")
    groups = partial.reshape(n_rep, n_tp, share, partial.shape[1])

    def chunk(step):
        return lax.dynamic_index_in_dim(groups, (tp + step) % n_tp, 1, keepdims=False)

    total = chunk(0).astype(jnp.float32)
    for step in range(1, n_tp):
        total = total + shifted(chunk(step), "tp", step).astype(jnp.float32)
    own = total[0]
    for step in range(1, n_rep):
        own = own + shifted(total[step].astype(jnp.bfloat16), "rep", -step).astype(jnp.float32)
    return own


def local(
    tokens,
    mix_gain,
    value_weight,
    outer_gate_weight,
    inner_gate_weight,
    conv_taps,
    mix_out_weight,
    ffn_gain,
    gate_weight,
    up_weight,
    down_weight,
):
    row_count = tokens.shape[0]
    share = row_count // lax.axis_size("tp")
    seq_len = row_count // SEQ_GRP
    n_rep, rep = lax.axis_size("rep"), lax.axis_index("rep")

    def part(array, axis):
        size = array.shape[axis] // n_rep
        return lax.dynamic_slice_in_dim(array, rep * size, size, axis)

    own_tokens = lax.dynamic_slice_in_dim(tokens, lax.axis_index("tp") * share, share, 0)
    conv_in = jnp.concatenate(
        [part(w, 1) for w in (value_weight, outer_gate_weight, inner_gate_weight)], axis=1
    )
    conv_full = lax.all_gather(conv_in, "fs", axis=0, tiled=True)
    mix_out_full = lax.all_gather(part(mix_out_weight, 0), "fs", axis=1, tiled=True)
    ffn_in = jnp.concatenate([part(w, 1) for w in (gate_weight, up_weight)], axis=1)
    ffn_full = lax.all_gather(ffn_in, "fs", axis=0, tiled=True)
    down_full = lax.all_gather(part(down_weight, 0), "fs", axis=1, tiled=True)

    normed = rms_norm(tokens, mix_gain)
    own_normed = lax.dynamic_slice_in_dim(normed, lax.axis_index("tp") * share, share, 0)
    rows = jnp.concatenate([normed] + [spread(b, "tp") for b in by_rep(own_normed)[1:]])
    proj = jnp.dot(rows, conv_full, preferred_element_type=jnp.float32).astype(jnp.bfloat16)
    value_proj, outer_proj, inner_proj = jnp.split(proj, 3, axis=1)
    mixed = short_conv(value_proj, outer_proj, inner_proj, part(conv_taps, 1), seq_len)
    mix_total = reduce_rows(
        jnp.dot(mixed, mix_out_full, preferred_element_type=jnp.float32).astype(jnp.bfloat16), share
    )
    after_mix = (own_tokens.astype(jnp.float32) + mix_total).astype(jnp.bfloat16)
    block_rows = group_rows(rms_norm(after_mix, ffn_gain))
    both = jnp.dot(block_rows, ffn_full, preferred_element_type=jnp.float32)
    gate_proj, up_proj = jnp.split(both, 2, axis=1)
    hidden = (jax.nn.silu(gate_proj) * up_proj).astype(jnp.bfloat16)
    ffn_total = reduce_rows(
        jnp.dot(hidden, down_full, preferred_element_type=jnp.float32).astype(jnp.bfloat16), share
    )
    finished = (after_mix.astype(jnp.float32) + ffn_total).astype(jnp.bfloat16)
    return spread(finished, "tp")


def solution(mesh):
    placed = (
        P(("rep", "fs"), None),
        P(),
        P("fs", "tp"),
        P("fs", "tp"),
        P("fs", "tp"),
        P(None, "tp"),
        P("tp", "fs"),
        P(),
        P("fs", "tp"),
        P("fs", "tp"),
        P("tp", "fs"),
    )
    return jax.shard_map(
        local, mesh=mesh, in_specs=placed, out_specs=P(("rep", "fs"), None), check_vma=False
    )
```

```python
import jax
import jax.numpy as jnp
from jax import lax
from jax.experimental import pallas as pl
from jax.experimental.pallas import tpu as pltpu
from jax.sharding import PartitionSpec as P

SEQ_GRP = 2


EPS = 1e-05


def rms_norm(values, gain):
    floats = values.astype(jnp.float32)
    scaled = floats * lax.rsqrt(jnp.mean(floats * floats, axis=-1, keepdims=True) + EPS)
    return (scaled * gain.astype(jnp.float32)).astype(jnp.bfloat16)


def short_conv(value_proj, outer_proj, inner_proj, conv_taps, seq_len):
    mixed_in = inner_proj.astype(jnp.float32) * value_proj.astype(jnp.float32)
    count_rows = mixed_in.shape[0]
    position = (jnp.arange(count_rows, dtype=jnp.int32) % seq_len)[:, None]
    zero_row = jnp.zeros((1, mixed_in.shape[1]), jnp.float32)
    back_one = jnp.where(position >= 1, jnp.concatenate([zero_row, mixed_in[:-1]], axis=0), 0.0)
    back_two = jnp.where(
        position >= 2, jnp.concatenate([zero_row, zero_row, mixed_in[:-2]], axis=0), 0.0
    )
    taps = conv_taps.astype(jnp.float32)
    convolved = taps[0] * back_two + taps[1] * back_one + taps[2] * mixed_in
    return (outer_proj.astype(jnp.float32) * convolved).astype(jnp.bfloat16)


def shifted(values, axis, step):
    size = lax.axis_size(axis)
    return lax.ppermute(values, axis, [(i, (i + step) % size) for i in range(size)])


def spread(block, axis):
    size, me, rows = lax.axis_size(axis), lax.axis_index(axis), block.shape[0]
    if size == 2:
        other = shifted(block, axis, 1)
        first = me == 0
        return jnp.concatenate([jnp.where(first, block, other), jnp.where(first, other, block)])
    whole = jnp.zeros((size * rows,) + block.shape[1:], block.dtype)
    for step in range(size):
        piece = block if step == 0 else shifted(block, axis, step)
        whole = lax.dynamic_update_slice_in_dim(whole, piece, (me - step) % size * rows, 0)
    return whole


WIDTH = 2
LONGEST_LINE = 4


def gather_kernel(depth, block_ref, whole_ref, send_sems, recv_sems, own_sem):
    me = lax.axis_index("fs")
    place, side = me // WIDTH, me % WIDTH
    rows = block_ref.shape[0]

    def slot(source_place, source_side):
        start = (source_place * WIDTH + source_side) * rows
        return whole_ref.at[pl.ds(pl.multiple_of(start, 16), rows), :]

    def copy(kind, step, source_place, to_place, to_side, first, source_side=None):
        landing = slot(source_place, side if source_side is None else source_side)
        return pltpu.make_async_remote_copy(
            src_ref=block_ref if first else landing,
            dst_ref=landing,
            send_sem=send_sems.at[kind, step],
            recv_sem=recv_sems.at[kind, step],
            device_id={"fs": to_place * WIDTH + to_side},
            device_id_type=pl.DeviceIdType.MESH,
        )

    def up(step):
        return copy(0, step, place - (step - 1), place + 1, side, step == 1)

    def up_came(step):
        return copy(0, step, place - step, place, 1 - side, False)

    def down(step):
        return copy(1, step, place + (step - 1), place - 1, side, step == 1)

    def down_came(step):
        return copy(1, step, place + step, place, 1 - side, False)

    def over(kind, step):
        source = place - step if kind == 2 else place + step
        return copy(kind, step, source, place, 1 - side, step == 0)

    def over_came(kind, step):
        source = place - step if kind == 2 else place + step
        return copy(kind, step, source, place, 1 - side, False, 1 - side)

    has_up, has_down = place < depth - 1, place > 0

    barrier = pltpu.get_barrier_semaphore()

    def greet(to):
        pl.semaphore_signal(
            barrier, inc=1, device_id={"fs": to}, device_id_type=pl.DeviceIdType.MESH
        )

    greet(place * WIDTH + 1 - side)
    pl.when(has_up)(lambda: greet((place + 1) * WIDTH + side))
    pl.when(has_down)(lambda: greet((place - 1) * WIDTH + side))
    pl.semaphore_wait(barrier, 1 + has_up.astype(jnp.int32) + has_down.astype(jnp.int32))

    pl.when(has_up)(lambda: up(1).start())
    pl.when(has_down)(lambda: down(1).start())
    over(2, 0).start()
    own = pltpu.make_async_copy(block_ref, slot(place, side), own_sem)
    own.start()

    for step in range(1, depth):

        @pl.when(place >= step)
        def _(step=step):
            up_came(step).wait_recv()
            if step + 1 < depth:
                pl.when(has_up)(lambda: up(step + 1).start())
            over(2, step).start()

        @pl.when(place + step < depth)
        def _(step=step):
            down_came(step).wait_recv()
            if step + 1 < depth:
                pl.when(has_down)(lambda: down(step + 1).start())
            over(3, step).start()

    own.wait()
    over(2, 0).wait_send()
    over_came(2, 0).wait_recv()
    for step in range(1, depth):
        pl.when((place >= step - 1) & has_up)(lambda step=step: up(step).wait_send())
        pl.when((place + step - 1 < depth) & has_down)(lambda step=step: down(step).wait_send())

        @pl.when(place >= step)
        def _(step=step):
            over(2, step).wait_send()
            over_came(2, step).wait_recv()

        @pl.when(place + step < depth)
        def _(step=step):
            over(3, step).wait_send()
            over_came(3, step).wait_recv()


def gather_fs(block):
    size = lax.axis_size("fs")
    depth = size // WIDTH
    rows, cols = block.shape
    if size % WIDTH or depth > LONGEST_LINE or rows % 16 or cols % 128:
        return lax.all_gather(block, "fs", axis=0, tiled=True)
    moved = size * rows * cols * 2
    return pl.pallas_call(
        lambda *refs: gather_kernel(depth, *refs),
        out_shape=jax.ShapeDtypeStruct((size * rows, cols), block.dtype),
        in_specs=[pl.BlockSpec(memory_space=pl.ANY)],
        out_specs=pl.BlockSpec(memory_space=pl.ANY),
        scratch_shapes=[
            pltpu.SemaphoreType.DMA((4, depth)),
            pltpu.SemaphoreType.DMA((4, depth)),
            pltpu.SemaphoreType.DMA,
        ],
        compiler_params=pltpu.CompilerParams(collective_id=0, has_side_effects=True),
        cost_estimate=pl.CostEstimate(flops=0, bytes_accessed=40 * moved, transcendentals=0),
        name="gather_mixer_weights",
    )(block)


def by_rep(block):
    return [block] + [shifted(block, "rep", step) for step in range(1, lax.axis_size("rep"))]


def group_rows(share_block):
    return jnp.concatenate([spread(block, "tp") for block in by_rep(share_block)])


def reduce_rows(partial, share):
    n_tp, tp, n_rep = lax.axis_size("tp"), lax.axis_index("tp"), lax.axis_size("rep")
    groups = partial.reshape(n_rep, n_tp, share, partial.shape[1])

    def chunk(step):
        return lax.dynamic_index_in_dim(groups, (tp + step) % n_tp, 1, keepdims=False)

    total = chunk(0).astype(jnp.float32)
    for step in range(1, n_tp):
        total = total + shifted(chunk(step), "tp", step).astype(jnp.float32)
    own = total[0]
    for step in range(1, n_rep):
        own = own + shifted(total[step].astype(jnp.bfloat16), "rep", -step).astype(jnp.float32)
    return own


def dot_t(left, right):
    return lax.dot_general(
        left, right, (((1,), (1,)), ((), ())), preferred_element_type=jnp.float32
    )


def local(
    tokens,
    mix_gain,
    value_weight,
    outer_gate_weight,
    inner_gate_weight,
    conv_taps,
    mix_out_weight,
    ffn_gain,
    gate_weight,
    up_weight,
    down_weight,
):
    row_count = tokens.shape[0]
    share = row_count // lax.axis_size("tp")
    seq_len = row_count // SEQ_GRP
    n_rep, rep = lax.axis_size("rep"), lax.axis_index("rep")

    def part(array, axis):
        size = array.shape[axis] // n_rep
        return lax.dynamic_slice_in_dim(array, rep * size, size, axis)

    own_tokens = lax.dynamic_slice_in_dim(tokens, lax.axis_index("tp") * share, share, 0)
    mix_in = jnp.concatenate(
        [part(w, 1) for w in (value_weight, outer_gate_weight, inner_gate_weight)]
        + [part(mix_out_weight, 0).T],
        axis=1,
    )
    mix_full = gather_fs(mix_in)
    channels = mix_out_weight.shape[0] // n_rep
    ffn_in = jnp.concatenate([part(w, 1) for w in (gate_weight, up_weight)], axis=1)
    ffn_full = lax.all_gather(ffn_in, "fs", axis=0, tiled=True)
    down_full = lax.all_gather(part(down_weight, 0), "fs", axis=1, tiled=True)

    normed = rms_norm(tokens, mix_gain)
    own_normed = lax.dynamic_slice_in_dim(normed, lax.axis_index("tp") * share, share, 0)
    received, mix_full = lax.optimization_barrier((by_rep(own_normed)[1:], mix_full))
    conv_full, mix_out_full = mix_full[:, : 3 * channels], mix_full[:, 3 * channels :]
    rows = jnp.concatenate([normed] + [spread(b, "tp") for b in received])
    proj = jnp.dot(rows, conv_full, preferred_element_type=jnp.float32).astype(jnp.bfloat16)
    value_proj, outer_proj, inner_proj = jnp.split(proj, 3, axis=1)
    mixed = short_conv(value_proj, outer_proj, inner_proj, part(conv_taps, 1), seq_len)
    mix_total = reduce_rows(
        dot_t(mixed, mix_out_full).astype(jnp.bfloat16), share
    )
    after_mix = (own_tokens.astype(jnp.float32) + mix_total).astype(jnp.bfloat16)
    block_rows = group_rows(rms_norm(after_mix, ffn_gain))
    both = jnp.dot(block_rows, ffn_full, preferred_element_type=jnp.float32)
    gate_proj, up_proj = jnp.split(both, 2, axis=1)
    hidden = (jax.nn.silu(gate_proj) * up_proj).astype(jnp.bfloat16)
    ffn_total = reduce_rows(
        jnp.dot(hidden, down_full, preferred_element_type=jnp.float32).astype(jnp.bfloat16), share
    )
    finished = (after_mix.astype(jnp.float32) + ffn_total).astype(jnp.bfloat16)
    return spread(finished, "tp")


def solution(mesh):
    placed = (
        P(("rep", "fs"), None),
        P(),
        P("fs", "tp"),
        P("fs", "tp"),
        P("fs", "tp"),
        P(None, "tp"),
        P("tp", "fs"),
        P(),
        P("fs", "tp"),
        P("fs", "tp"),
        P("tp", "fs"),
    )
    return jax.shard_map(
        local, mesh=mesh, in_specs=placed, out_specs=P(("rep", "fs"), None), check_vma=False
    )
```
